32 devices in a mesh: ep: 4 (over y, x), tp: 8 (over z, core).
Axes of the slice: x: 2, y: 2, z: 4, core: 2. Of those that a mesh axis runs over, the one named last changes fastest.
Arguments:
- queries: bfloat16 [2048, 16, 128], P('ep', 'tp'), may hold values from -125 to 125
- keys: bfloat16 [2048, 16, 128], P('ep', 'tp'), may hold values from -9 to 9
- values: bfloat16 [2048, 16, 128], P('ep', 'tp'), may hold values from -6 to 6
- mixing: float32 [16], P('tp'), may hold values from 0.3 to 0.8
- head_gain: float32 [128], replicated, may hold values from 0.1 to 1.9
- out_weight: bfloat16 [16, 128, 2048], P('tp'), may hold values from -0.125 to 0.125
- tokens_b: bfloat16 [4096, 2048], P(('ep', 'tp')), may hold values from -6 to 6
- norm_gain: float32 [2048], replicated, may hold values from 0.1 to 1.9
- expert_ids: int32 [4096, 2], P(('ep', 'tp')), may hold values from 0 to 3, all different within a row; in each aligned block of 128 rows (0 to 127, 128 to 255, ...) at most 96 rows name the same one
- group_gate: float32 [4096], P(('ep', 'tp')), may hold values from 0.2 to 1
- expert_gate: float32 [4096, 2], P(('ep', 'tp')), may hold values from 0.1 to 0.9
- gate_weight: bfloat16 [4, 2048, 1024], P('ep', None, 'tp'), may hold values from -0.125 to 0.125
- up_weight: bfloat16 [4, 2048, 1024], P('ep', None, 'tp'), may hold values from -0.125 to 0.125
- down_weight: bfloat16 [4, 2048, 1024], P('ep', None, 'tp'), may hold values from -0.1875 to 0.1875
Outputs:
- mixed: bfloat16 [2048, 2048], P(('ep', 'tp'))
- routed: bfloat16 [4096, 2048], P(('ep', 'tp'))
The draws below stay inside these ranges and needn't reach their ends.
Inputs may be any that keep to these rules, and one draw needn't show every extreme that they name: `expert_ids`: within each aligned block of 128 rows, no expert is named by more than 96 rows, and some block has an expert named by exactly 96 rows.
All inputs are finite; a program needn't handle non-finite values.
Results may differ from the reference program's by a relative error of at most 0.019.
Values may be sent and summed in bfloat16 or wider, within the bound.
A program may use at most 192 MiB of HBM per device.

```python
import math
import jax
import jax.numpy as jnp
import numpy as np
from jax import lax

D = 2048
HEADS = 16
HEAD = 64
VAL = 128
FF = 1024
TOP = 2
EXPERTS = 4
SEQ_DEV = 512
LENGTH = 2048
TOK_DEV = 128
TOKENS_B = 4096
CAP = 96
N_EP = 4
N_TP = 8


def paired_fields(key):
    query_seed = jax.random.fold_in(key, 11)
    key_seed = jax.random.fold_in(key, 12)
    query_field = jnp.clip(jax.random.normal(query_seed, (LENGTH, HEADS, 2 * HEAD), jnp.float32), -5.0, 5.0)
    key_field = 1.75 * jnp.clip(jax.random.normal(key_seed, (LENGTH, HEADS, 2 * HEAD), jnp.float32), -5.0, 5.0)
    return (query_field, key_field)


def draw_queries(key, part):
    return paired_fields(key)[0].astype(jnp.bfloat16)


def draw_keys(key, part):
    return paired_fields(key)[1].astype(jnp.bfloat16)


def levels(rng, shape, pieces, smallest, top_value):
    level = 1.0
    for axis_at, parts in pieces:
        heights = jax.random.uniform(jax.random.fold_in(jax.random.fold_in(rng, 6), axis_at), (parts,), jnp.float32, smallest / len(pieces), top_value / len(pieces))
        level = level * jnp.repeat(jnp.exp(heights), shape[axis_at] // parts).reshape((-1,) + (1,) * (len(shape) - 1 - axis_at))
    return level


def shared_out(key, own, number, rows, count, top, most, lean):
    ranking = jax.random.permutation(key, count)
    packed, common = load_shares(count, rows * top, most, lean, True), load_shares(count, rows * top, most, lean, False)
    places = jnp.arange(count)

    def named(lengths, offset_by):
        used = int((lengths > 0).sum())
        fixed = max(1, used // 4)
        moved = fixed + (places - fixed + offset_by * (used - fixed)) % max(1, count - fixed)
        return jnp.zeros((count,), jnp.int32).at[ranking[jnp.where(places < fixed, places, moved)]].set(jnp.asarray(lengths, jnp.int32))

    lengths = jnp.where(number % 4 == 0, named(packed, number // 4), named(common, number - number // 4 - 1))
    mixed = jax.random.permutation(jax.random.fold_in(own, 3), count)
    source_of, taker = mixed[0:count // 2 * 2:2], mixed[1:count // 2 * 2:2]
    margin = jnp.minimum(lengths[source_of] - 1, most - lengths[taker]) // 2
    margin = jnp.where((source_of == ranking[0]) | (taker == ranking[0]) | (lengths[taker] == 0), 0, jnp.maximum(margin, 0))
    moved = jax.random.randint(jax.random.fold_in(own, 4), (count // 2,), 0, 1 << 20) % (margin + 1)
    lengths = lengths.at[source_of].add(-moved).at[taker].add(moved)
    items = jnp.searchsorted(jnp.cumsum(lengths), jnp.arange(rows * top), side="right").astype(jnp.int32)
    table = items.reshape(top, rows).T
    table = table[jax.random.permutation(jax.random.fold_in(own, 1), rows)]
    offset_by = jax.random.randint(jax.random.fold_in(own, 2), (rows, 1), 0, top)
    return jnp.take_along_axis(table, (jnp.arange(top)[None, :] + offset_by) % top, axis=1)


def load_shares(count, total, bound, lean, full):
    loads = [(1 << 20) // math.isqrt(standing ** lean) + 1 for standing in range(1, count + 1)]
    largest = bound if full else min(bound, max(-(-total // count), total * loads[0] // sum(loads)))
    least = 1 if total - largest >= count - 1 else 0
    given, spare = [largest] + [least] * (count - 1), total - largest - least * (count - 1)
    while spare > 0:
        free = [i for i in range(1, count) if given[i] < largest] or [i for i in range(1, count) if given[i] < bound]
        pool, budget = sum([loads[i] for i in free]), spare
        for i in free:
            extra = min(bound - given[i], max(1, budget * loads[i] // pool), spare)
            given[i] = given[i] + extra
            spare = spare - extra
    return np.array(given)


def scatter_about(stream_key, shape, scale, limit, cuts=(), kind=jnp.bfloat16):
    factor_of = levels(stream_key, shape, cuts, -0.22, 0.18) if cuts else 1.0
    array = jax.random.normal(stream_key, shape, jnp.float32) * scale * factor_of
    return jnp.minimum(jnp.maximum(array, -limit), limit).astype(kind)


def setup_inputs(seed: int = 0) -> dict:
    arg_keys = jax.random.split(jax.random.key(seed), 15)
    queries = draw_queries(jax.random.fold_in(arg_keys[14], 71), 0)
    keys = draw_keys(jax.random.fold_in(arg_keys[14], 71), 0)
    values = scatter_about(arg_keys[2], (LENGTH, HEADS, VAL), 1.0, 6.0, ((0, 4), (1, 8)))
    mixing = jnp.clip(0.3 + 0.5 * jax.random.uniform(arg_keys[3], (HEADS,), jnp.float32) ** levels(arg_keys[3], (HEADS,), ((0, 8),), -0.2, 0.2), 0.3, 0.8)
    head_gain = jnp.clip(1.0 + 0.18 * jax.random.normal(arg_keys[4], (VAL,), jnp.float32), 0.1, 1.9)
    out_weight = scatter_about(arg_keys[5], (HEADS, VAL, D), (HEADS * VAL) ** -0.5, 0.125, ((0, 8),))
    tokens_b = scatter_about(arg_keys[6], (TOKENS_B, D), 1.0, 6.0, ((0, 32),))
    norm_gain = jnp.clip(1.0 + 0.18 * jax.random.normal(arg_keys[7], (D,), jnp.float32), 0.1, 1.9)
    expert_ids_keys = jax.random.split(jax.random.fold_in(arg_keys[8], 1), TOKENS_B // TOK_DEV)
    expert_ids_turns = jax.random.permutation(jax.random.fold_in(arg_keys[8], 3), TOKENS_B // TOK_DEV)
    expert_ids = jax.vmap(lambda own, number: shared_out(jax.random.fold_in(arg_keys[8], 2), own, number, TOK_DEV, EXPERTS, TOP, CAP, 0))(expert_ids_keys, expert_ids_turns).reshape((TOKENS_B, TOP))
    group_gate = jnp.clip(jnp.exp(math.log(1.0) - 1.609438 * jax.random.uniform(arg_keys[9], (TOKENS_B,), jnp.float32) ** levels(arg_keys[9], (TOKENS_B,), ((0, 32),), -0.2, 0.2)), 0.2, 1.0)
    expert_gate = jnp.clip(0.1 + 0.79999997 * jax.random.uniform(arg_keys[10], (TOKENS_B, TOP), jnp.float32) ** levels(arg_keys[10], (TOKENS_B, TOP), ((0, 32),), -0.2, 0.2), 0.1, 0.9)
    gate_weight = scatter_about(arg_keys[11], (EXPERTS, D, FF), D ** -0.5, 0.125, ((0, 4), (2, 8)))
    up_weight = scatter_about(arg_keys[12], (EXPERTS, D, FF), D ** -0.5, 0.125, ((0, 4), (2, 8)))
    down_weight = scatter_about(arg_keys[13], (EXPERTS, D, FF), FF ** -0.5, 0.1875, ((0, 4), (2, 8)))
    return dict(queries=queries, keys=keys, values=values, mixing=mixing, head_gain=head_gain, out_weight=out_weight, tokens_b=tokens_b, norm_gain=norm_gain, expert_ids=expert_ids, group_gate=group_gate, expert_gate=expert_gate, gate_weight=gate_weight, up_weight=up_weight, down_weight=down_weight)


def attend_head(inputs, head_gain):
    query_head, key_head, value_head, weight_two = inputs
    positions = lax.iota(jnp.int32, LENGTH)
    score_scale = 1.0 / math.sqrt(HEAD)

    def one_block(block_index):
        query_block = lax.dynamic_slice_in_dim(query_head, block_index * SEQ_DEV, SEQ_DEV, 0)
        query_pos = block_index * SEQ_DEV + lax.iota(jnp.int32, SEQ_DEV)
        allowed = positions[None, :] <= query_pos[:, None]
        results = []
        for map_index in range(2):
            offset = map_index * HEAD
            scores = jnp.dot(query_block[:, offset:offset + HEAD], key_head[:, offset:offset + HEAD].T, preferred_element_type=jnp.float32) * score_scale
            scores = jnp.where(allowed, scores, -1e+30)
            row_top = lax.optimization_barrier(jnp.max(scores, axis=1, keepdims=True))
            expo = jnp.exp(scores - row_top)
            row_sum = lax.optimization_barrier(jnp.sum(expo, axis=1, keepdims=True))
            numerator = jnp.dot(expo.astype(jnp.bfloat16), value_head, preferred_element_type=jnp.float32)
            results.append(numerator / row_sum)
        diff = results[0] - weight_two * results[1]
        normed = diff * lax.rsqrt(lax.optimization_barrier(jnp.mean(diff * diff, axis=1, keepdims=True)) + 1e-05) * head_gain
        return normed.astype(jnp.bfloat16)
    blocks = lax.map(one_block, jnp.arange(N_EP, dtype=jnp.int32))
    return blocks.reshape(LENGTH, VAL)

def expert_apply(inputs):
    expert_rows, w_gate, w_up, w_down = inputs
    gate_part = jnp.dot(expert_rows, w_gate, preferred_element_type=jnp.float32)
    up_part = jnp.dot(expert_rows, w_up, preferred_element_type=jnp.float32)
    hidden = (jax.nn.silu(gate_part) * up_part).astype(jnp.bfloat16)
    return jnp.dot(hidden, w_down.T, preferred_element_type=jnp.float32).astype(jnp.bfloat16)

def block_slots(block_ids):
    one_hot = (block_ids[:, None] == jnp.arange(EXPERTS, dtype=jnp.int32)[None, :]).astype(jnp.int32)
    slot_rank = lax.optimization_barrier(jnp.sum((jnp.cumsum(one_hot, axis=0) - one_hot) * one_hot, axis=1))
    slot_index = block_ids * CAP + slot_rank
    owners = jnp.full((EXPERTS * CAP,), TOK_DEV, jnp.int32)
    owners = owners.at[slot_index].set(jnp.arange(TOK_DEV * TOP, dtype=jnp.int32) // TOP)
    return (slot_index, owners)

def reference(queries, keys, values, mixing, head_gain, out_weight, tokens_b, norm_gain, expert_ids, group_gate, expert_gate, gate_weight, up_weight, down_weight):
    attended = lax.map(lambda inputs: attend_head(inputs, head_gain), (jnp.transpose(queries, (1, 0, 2)), jnp.transpose(keys, (1, 0, 2)), jnp.transpose(values, (1, 0, 2)), mixing))
    group_heads = HEADS // N_TP
    summed = jnp.zeros((LENGTH, D), jnp.float32)
    for group in range(N_TP):
        lower_head = group * group_heads
        part = jnp.einsum('hqe,hed->qd', attended[lower_head:lower_head + group_heads].astype(jnp.float32), out_weight[lower_head:lower_head + group_heads].astype(jnp.float32))
        rounded = lax.optimization_barrier(part.astype(jnp.bfloat16))
        summed = summed + rounded.astype(jnp.float32)
    mixed = summed.astype(jnp.bfloat16)
    tokens_f = tokens_b.astype(jnp.float32)
    normed = (tokens_f * lax.rsqrt(lax.optimization_barrier(jnp.mean(tokens_f * tokens_f, axis=1, keepdims=True)) + 1e-06) * norm_gain).astype(jnp.bfloat16)
    block_count = N_EP * N_TP
    slot_index, owners = jax.vmap(block_slots)(expert_ids.reshape(block_count, TOK_DEV * TOP))
    padded = jnp.concatenate([normed.reshape(block_count, TOK_DEV, D), jnp.zeros((block_count, 1, D), jnp.bfloat16)], axis=1)
    buffers = jnp.take_along_axis(padded, owners[:, :, None], axis=1)
    per_expert = jnp.transpose(buffers.reshape(block_count, EXPERTS, CAP, D), (1, 0, 2, 3))
    per_expert = per_expert.reshape(EXPERTS, block_count * CAP, D)
    results = lax.map(expert_apply, (per_expert, gate_weight, up_weight, down_weight))
    results = jnp.transpose(results.reshape(EXPERTS, block_count, CAP, D), (1, 0, 2, 3))
    results = results.reshape(block_count, EXPERTS * CAP, D)
    picked = jnp.take_along_axis(results, slot_index[:, :, None], axis=1)
    picked = picked.reshape(TOKENS_B, TOP, D).astype(jnp.float32)
    route_weight = group_gate[:, None] * expert_gate
    routed = lax.optimization_barrier(jnp.sum(route_weight[:, :, None] * picked, axis=1)).astype(jnp.bfloat16)
    return (mixed, routed)
```

```python
import functools
import math

import jax
import jax.numpy as jnp
from jax import lax
from jax.experimental import pallas as pl
from jax.experimental.pallas import tpu as pltpu
from jax.sharding import PartitionSpec as P

HEAD = 64
CHUNKS = 4
F32 = jnp.float32
BF16 = jnp.bfloat16
MESH = pl.DeviceIdType.MESH
NT = (((1,), (1,)), ((), ()))


def kernel(
    ep,
    tp,
    mix_ref,
    q_ref,
    kv_ref,
    gain_ref,
    ow_ref,
    tok_ref,
    norm_ref,
    ids_ref,
    group_ref,
    gates_ref,
    gate_ref,
    up_ref,
    dn_ref,
    mixed_ref,
    routed_ref,
    kv_all,
    w_gu,
    w_dn,
    rows_x,
    acc,
    hid,
    give,
    take,
    back,
    ret,
    att,
    part,
    pair,
    chip_sum,
    landed,
    line_out,
    out_ref,
    place_ref,
    route_ref,
    local_sem,
    kv_s,
    kv_r,
    x_s,
    x_r,
    xp_s,
    xp_r,
    gu_s,
    gu_r,
    dn_s,
    dn_r,
    pr_s,
    pr_r,
    rs_s,
    rs_r,
    o_s,
    o_r,
    b_s,
    b_r,
):
    chips = tp // 2
    me = lax.axis_index("ep")
    mine = lax.axis_index("tp")
    z = mine // 2
    core = mine % 2
    other = z * 2 + 1 - core
    heads, length, wide = q_ref.shape
    cap = out_ref.shape[1]
    half = ep * cap
    unit = dn_ref.shape[2]
    step = dn_ref.shape[1]
    joined = gate_ref.shape[1] != unit

    def remote(src, dst, send, recv, target):
        return pltpu.make_async_remote_copy(
            src_ref=src,
            dst_ref=dst,
            send_sem=send,
            recv_sem=recv,
            device_id=target,
            device_id_type=MESH,
        )

    barrier = pltpu.get_barrier_semaphore()
    for s in range(1, ep):
        pl.semaphore_signal(
            barrier, inc=1, device_id={"ep": (me + s) % ep}, device_id_type=MESH
        )
    for s in range(1, tp):
        pl.semaphore_signal(
            barrier, inc=1, device_id={"tp": (mine + s) % tp}, device_id_type=MESH
        )
    pl.semaphore_wait(barrier, ep + tp - 2)

    def gu_copy(src, side):
        target = (z + 1 - 2 * side) * 2 + core
        return remote(
            w_gu.at[src], w_gu.at[src], gu_s.at[side, src], gu_r.at[src], {"tp": target}
        )

    def dn_copy(src, c, side):
        target = (z + 1 - 2 * side) * 2 + core
        return remote(
            w_dn.at[src, c],
            w_dn.at[src, c],
            dn_s.at[side, src, c],
            dn_r.at[src, c],
            {"tp": target},
        )

    def has_next(side):
        return (z < chips - 1) if side == 0 else (z > 0)

    def source(k, side):
        return z - k if side == 0 else z + k

    def exists(k, side):
        return (z >= k) if side == 0 else (z + k <= chips - 1)

    own = [
        pltpu.make_async_copy(
            gate_ref, w_gu.at[z] if joined else w_gu.at[z, :, pl.ds(0, unit)], local_sem.at[0]
        ),
        pltpu.make_async_copy(dn_ref, w_dn.at[z], local_sem.at[1]),
        pltpu.make_async_copy(kv_ref, kv_all.at[0], local_sem.at[2]),
        pltpu.make_async_copy(out_ref.at[0], rows_x.at[pl.ds(0, cap)], local_sem.at[3]),
    ]
    if not joined:
        own.append(
            pltpu.make_async_copy(up_ref, w_gu.at[z, :, pl.ds(unit, unit)], local_sem.at[4])
        )
    for copy in own[:3] + own[4:]:
        copy.start()

    def kv_copy(s):
        return remote(kv_ref, kv_all.at[s], kv_s.at[s], kv_r.at[s], {"ep": lax.rem(me + s, ep)})

    for s in range(1, ep):
        pl.when(me + s < ep)(lambda s=s: kv_copy(s).start())
    own[0].wait()
    if not joined:
        own[4].wait()
    for side in range(2):
        pl.when(has_next(side))(lambda side=side: gu_copy(z, side).start())
    own[1].wait()
    for side in range(2):

        @pl.when(has_next(side))
        def _(side=side):
            for c in range(CHUNKS):
                dn_copy(z, c, side).start()

    def x_copy(s):
        return remote(
            out_ref.at[s],
            rows_x.at[pl.ds(s * cap, cap)],
            x_s.at[s],
            x_r.at[s],
            {"ep": lax.rem(me + s, ep)},
        )

    def xp_copy(s):
        src = rows_x.at[pl.ds(s * cap, cap)]
        dst = rows_x.at[pl.ds(half + s * cap, cap)]
        return remote(src, dst, xp_s.at[s], xp_r.at[s], {"tp": other})

    def pass_gu(k):
        for side in range(2):

            @pl.when(exists(k, side) & has_next(side))
            def _(side=side):
                src = source(k, side)
                gu_copy(src, side).wait_recv()
                gu_copy(src, side).start()

    def pass_dn(k, c):
        for side in range(2):

            @pl.when(exists(k, side) & has_next(side))
            def _(side=side):
                src = source(k, side)
                dn_copy(src, c, side).wait_recv()
                dn_copy(src, c, side).start()

    tokens = tok_ref[...].astype(F32)
    normed = (
        tokens
        * lax.rsqrt(jnp.mean(tokens * tokens, axis=1, keepdims=True) + 1e-06)
        * norm_ref[...]
    ).astype(BF16)
    local_rows = tok_ref.shape[0]
    relative = ids_ref[...] - me
    relative = jnp.where(relative < 0, relative + ep, relative)
    expert_lane = lax.broadcasted_iota(jnp.int32, (local_rows, ep), 1)
    named = jnp.zeros((local_rows, ep), F32)
    route = jnp.zeros((local_rows, ep), F32)
    for k in range(ids_ref.shape[1]):
        hit = expert_lane == relative[:, k : k + 1]
        named = jnp.where(hit, 1.0, named)
        route = route + jnp.where(hit, group_ref[...] * gates_ref[:, k : k + 1], 0.0)
    route_ref[...] = route
    square = (local_rows, local_rows)
    before = jnp.where(
        lax.broadcasted_iota(jnp.int32, square, 1) < lax.broadcasted_iota(jnp.int32, square, 0),
        1.0,
        0.0,
    ).astype(BF16)
    rank = jnp.dot(before, named.astype(BF16), preferred_element_type=F32)
    rank = jnp.where(named > 0.5, rank, -1.0).astype(jnp.int32)
    slot_lane = lax.broadcasted_iota(jnp.int32, (local_rows, cap), 1)
    for s in list(range(1, ep)) + [0]:
        place = jnp.where(rank[:, s : s + 1] == slot_lane, 1.0, 0.0).astype(BF16)
        place_ref[s] = place
        out_ref[s] = lax.dot_general(
            place, normed, (((0,), (0,)), ((), ())), preferred_element_type=F32
        ).astype(BF16)
        if s:
            x_copy(s).start()
    own[3].start()
    own[3].wait()
    xp_copy(0).start()

    own[2].wait()
    for s in range(1, ep):
        pl.when(me >= s)(lambda s=s: kv_copy(s).wait_recv())
    if chips > 2:
        pass_gu(1)
    tile = min(256, length)
    tiles = length // tile

    def attend(index, carry):
        h = index // tiles
        start = pl.multiple_of((index % tiles) * tile, tile)
        q = q_ref[h, pl.ds(start, tile), :]
        lane = lax.broadcasted_iota(jnp.int32, (tile, wide), 1)
        ratio = []
        for m in range(2):
            pick = (lane < HEAD) if m == 0 else (lane >= HEAD)
            q_map = jnp.where(pick, q, jnp.zeros_like(q))

            def visit(s, state, diagonal=False, q_map=q_map):
                top, total, value = state
                scores = lax.dot_general(
                    q_map, kv_all[s, h, :, :wide], NT, preferred_element_type=F32
                )
                if diagonal:
                    row = start + lax.broadcasted_iota(jnp.int32, scores.shape, 0)
                    col = lax.broadcasted_iota(jnp.int32, scores.shape, 1)
                    scores = jnp.where(col <= row, scores, -1e30)
                fresh = jnp.maximum(top, jnp.max(scores, axis=1, keepdims=True))
                shrink = jnp.exp(top - fresh)
                expo = jnp.exp(scores - fresh)
                total = total * shrink + jnp.sum(expo, axis=1, keepdims=True)
                value = value * shrink + jnp.dot(
                    expo.astype(BF16), kv_all[s, h, :, wide:], preferred_element_type=F32
                )
                return fresh, total, value

            state = (
                jnp.full((tile, 1), -1e30, F32),
                jnp.zeros((tile, 1), F32),
                jnp.zeros((tile, kv_ref.shape[2] - wide), F32),
            )
            state = visit(0, state, True)
            state = lax.fori_loop(1, me + 1, visit, state)
            ratio.append(state[2] / state[1])
        diff = ratio[0] - mix_ref[h] * ratio[1]
        scaled = diff * lax.rsqrt(jnp.mean(diff * diff, axis=1, keepdims=True) + 1e-05)
        att[h, pl.ds(start, tile), :] = (scaled * gain_ref[...]).astype(BF16)
        return carry

    lax.fori_loop(0, heads * tiles, attend, 0)

    block = length // tp

    def project(t, carry):
        rows = pl.ds(pl.multiple_of(t * 2 * block, 2 * block), 2 * block)
        total = 0.0
        for h in range(heads):
            total = total + jnp.dot(att[h, rows, :], ow_ref[h], preferred_element_type=F32)
        part[0, t] = total[:block].astype(BF16)
        part[1, t] = total[block:].astype(BF16)
        return carry

    lax.fori_loop(0, chips, project, 0)
    pair_copy = remote(part.at[1 - core], pair, pr_s, pr_r, {"tp": other})
    pair_copy.start()
    for s in range(1, ep):
        x_copy(s).wait_recv()
        xp_copy(s).start()
    pair_copy.wait_recv()

    def add_pair(t, carry):
        chip_sum[t] = (part[core, t].astype(F32) + pair[t].astype(F32)).astype(BF16)
        return carry

    lax.fori_loop(0, chips, add_pair, 0)

    def line_copy(side, t, first):
        return remote(
            chip_sum.at[t] if first else line_out.at[side, t],
            landed.at[side, t],
            rs_s.at[side, t],
            rs_r.at[side, t],
            {"tp": (z + 1 - 2 * side) * 2 + core},
        )

    def stage_each(k, do):
        for side in range(2):
            at = k if side == 0 else chips - 1 - k
            targets = range(chips - 1, k, -1) if side == 0 else range(chips - 1 - k)

            @pl.when(z == at)
            def _(side=side, targets=targets):
                for t in targets:
                    do(side, t, k == 0)

    def stage_send(side, t, first):
        copy = line_copy(side, t, first)
        if not first:
            copy.wait_recv()
            line_out[side, t] = (
                chip_sum[t].astype(F32) + landed[side, t].astype(F32)
            ).astype(BF16)
        copy.start()

    stage_each(0, stage_send)

    m_tile = 256 if (2 * half) % 256 == 0 else cap
    m_count = 2 * half // m_tile

    def hidden_of(src):
        def one(t, carry):
            rows = pl.ds(pl.multiple_of(t * m_tile, m_tile), m_tile)
            product = jnp.dot(rows_x[rows, :], w_gu[src], preferred_element_type=F32)
            gate = product[:, :unit]
            hid[src, rows, :] = (
                gate / (1.0 + jnp.exp(-gate)) * product[:, unit:]
            ).astype(BF16)
            return carry

        lax.fori_loop(0, m_count, one, 0)

    def down_of(src, c, first=False):
        def one(t, carry):
            rows = pl.ds(pl.multiple_of(t * m_tile, m_tile), m_tile)
            product = lax.dot_general(
                hid[src, rows, :], w_dn[src, c], NT, preferred_element_type=F32
            )
            if first:
                acc[c, rows, :] = product
            else:
                acc[c, rows, :] += product
            return carry

        lax.fori_loop(0, m_count, one, 0)

    def use_gu(k):
        for side in range(2):

            @pl.when(exists(k, side))
            def _(side=side):
                src = source(k, side)
                pl.when(jnp.logical_not(has_next(side)))(lambda: gu_copy(src, side).wait_recv())
                hidden_of(src)

    def use_dn(k, c):
        for side in range(2):

            @pl.when(exists(k, side))
            def _(side=side):
                src = source(k, side)
                pl.when(jnp.logical_not(has_next(side)))(
                    lambda: dn_copy(src, c, side).wait_recv()
                )
                down_of(src, c)

    last = chips - 1
    late = [k for k in (last - 2, last - 1) if k >= 1]
    for s in range(ep):
        xp_copy(s).wait_recv()
    hidden_of(z)
    for c in range(CHUNKS):
        down_of(z, c, True)
    for k in range(1, last):
        if k + 1 < last:
            pass_gu(k + 1)
        use_gu(k)
        if k < last - 2:
            for c in range(CHUNKS):
                pass_dn(k, c)
        elif k == late[0]:
            for c in range(CHUNKS):
                for near in late:
                    pass_dn(near, c)
        stage_each(k, stage_send)
        if k < last - 1:
            for c in range(CHUNKS):
                use_dn(k, c)
    if last > 0:
        use_gu(last)

    def give_copy(c):
        return remote(give.at[c], take.at[c], o_s.at[c], o_r.at[c], {"tp": other})

    def back_copy(c, s):
        return remote(
            back.at[c, s],
            ret.at[c, s],
            b_s.at[c, s],
            b_r.at[c, s],
            {"ep": lax.rem(me + ep - s, ep)},
        )

    def combine(c):
        total = 0.0
        for s in range(ep):
            if s == 0:
                block_rows = back[c, 0]
            else:
                back_copy(c, s).wait_recv()
                block_rows = ret[c, s]
            picked = jnp.dot(place_ref[s], block_rows, preferred_element_type=F32)
            total = total + route_ref[:, s : s + 1] * picked
        routed_ref[:, c * step : (c + 1) * step] = total.astype(BF16)

    for c in range(CHUNKS):
        for k in range(max(last - 1, 1), last + 1):
            use_dn(k, c)
        give[c] = acc[c, half:, :].astype(BF16)
        give_copy(c).start()
        give_copy(c).wait_recv()
        for s in range(ep):
            rows = slice(s * cap, (s + 1) * cap)
            back[c, s] = (acc[c, rows, :] + take[c, rows, :].astype(F32)).astype(BF16)
        for s in range(1, ep):
            back_copy(c, s).start()
        if c > 1:
            combine(c - 2)
    mixed_ref[...] = chip_sum[z]
    for side in range(2):

        @pl.when((z > 0) if side == 0 else (z < chips - 1))
        def _(side=side):
            line_copy(side, z, False).wait_recv()
            mixed_ref[...] = (
                mixed_ref[...].astype(F32) + landed[side, z].astype(F32)
            ).astype(BF16)

    for c in range(max(CHUNKS - 2, 0), CHUNKS):
        combine(c)

    for s in range(1, ep):
        pl.when(me + s < ep)(lambda s=s: kv_copy(s).wait_send())
        x_copy(s).wait_send()
    for s in range(ep):
        xp_copy(s).wait_send()
    for k in range(chips - 1):
        for side in range(2):

            @pl.when(exists(k, side) & has_next(side))
            def _(side=side, k=k):
                src = source(k, side)
                gu_copy(src, side).wait_send()
                for c in range(CHUNKS):
                    dn_copy(src, c, side).wait_send()

    pair_copy.wait_send()
    for k in range(chips - 1):
        stage_each(k, lambda side, t, first: line_copy(side, t, first).wait_send())
    for c in range(CHUNKS):
        give_copy(c).wait_send()
        for s in range(1, ep):
            back_copy(c, s).wait_send()


def per_device(
    queries,
    keys,
    values,
    mixing,
    head_gain,
    out_weight,
    tokens_b,
    norm_gain,
    expert_ids,
    group_gate,
    expert_gate,
    gate_weight,
    up_weight,
    down_weight,
):
    ep = lax.axis_size("ep")
    tp = lax.axis_size("tp")
    chips = tp // 2
    length, heads, wide = queries.shape
    val = values.shape[2]
    local_rows, width = tokens_b.shape
    top_count = expert_ids.shape[1]
    unit = gate_weight.shape[2]
    assert gate_weight.shape[0] == 1 and wide == 2 * HEAD
    capacity = 3 * local_rows * top_count // (2 * ep)
    cap = -(-capacity // 16) * 16
    step = width // CHUNKS

    scaled = (queries.astype(F32) * (1.0 / math.sqrt(HEAD))).astype(BF16).transpose(1, 0, 2)
    kv = jnp.concatenate([keys, values], axis=2).transpose(1, 0, 2)
    gate, up = gate_weight[0], up_weight[0]
    if unit % 128:
        gate = jnp.concatenate([gate, up], axis=1)
    half = ep * cap
    block = length // tp
    vmem = pl.BlockSpec(memory_space=pltpu.VMEM)
    dma = pltpu.SemaphoreType.DMA
    return pl.pallas_call(
        functools.partial(kernel, ep, tp),
        out_shape=(
            jax.ShapeDtypeStruct((block, width), BF16),
            jax.ShapeDtypeStruct((local_rows, width), BF16),
        ),
        in_specs=[pl.BlockSpec(memory_space=pltpu.SMEM)] + [vmem] * 12,
        out_specs=(vmem, vmem),
        scratch_shapes=[
            pltpu.VMEM((ep, heads, length, wide + val), BF16),
            pltpu.VMEM((chips, width, 2 * unit), BF16),
            pltpu.VMEM((chips, CHUNKS, step, unit), BF16),
            pltpu.VMEM((2 * half, width), BF16),
            pltpu.VMEM((CHUNKS, 2 * half, step), F32),
            pltpu.VMEM((chips, 2 * half, unit), BF16),
            pltpu.VMEM((CHUNKS, half, step), BF16),
            pltpu.VMEM((CHUNKS, half, step), BF16),
            pltpu.VMEM((CHUNKS, ep, cap, step), BF16),
            pltpu.VMEM((CHUNKS, ep, cap, step), BF16),
            pltpu.VMEM((heads, length, val), BF16),
            pltpu.VMEM((2, chips, block, width), BF16),
            pltpu.VMEM((chips, block, width), BF16),
            pltpu.VMEM((chips, block, width), BF16),
            pltpu.VMEM((2, chips, block, width), BF16),
            pltpu.VMEM((2, chips, block, width), BF16),
            pltpu.VMEM((ep, cap, width), BF16),
            pltpu.VMEM((ep, local_rows, cap), BF16),
            pltpu.VMEM((local_rows, ep), F32),
            dma((5,)),
            dma((ep,)),
            dma((ep,)),
            dma((ep,)),
            dma((ep,)),
            dma((ep,)),
            dma((ep,)),
            dma((2, chips)),
            dma((chips,)),
            dma((2, chips, CHUNKS)),
            dma((chips, CHUNKS)),
            dma,
            dma,
            dma((2, chips)),
            dma((2, chips)),
            dma((CHUNKS,)),
            dma((CHUNKS,)),
            dma((CHUNKS, ep)),
            dma((CHUNKS, ep)),
        ],
        compiler_params=pltpu.CompilerParams(
            collective_id=0, has_side_effects=True, vmem_limit_bytes=62 * 1024 * 1024
        ),
    )(
        mixing,
        scaled,
        kv,
        head_gain[None],
        out_weight,
        tokens_b,
        norm_gain[None],
        expert_ids,
        group_gate[:, None],
        expert_gate,
        gate,
        up,
        down_weight[0].reshape(CHUNKS, step, unit),
    )


def solution(mesh):
    placed = (
        P("ep", "tp", None),
        P("ep", "tp", None),
        P("ep", "tp", None),
        P("tp"),
        P(),
        P("tp", None, None),
        P(("ep", "tp"), None),
        P(),
        P(("ep", "tp"), None),
        P(("ep", "tp")),
        P(("ep", "tp"), None),
        P("ep", None, "tp"),
        P("ep", None, "tp"),
        P("ep", None, "tp"),
    )
    return jax.shard_map(
        per_device,
        mesh=mesh,
        in_specs=placed,
        out_specs=(P(("ep", "tp"), None), P(("ep", "tp"), None)),
        check_vma=False,
    )
```
